32 devices in a mesh: kv: 8 (over z, y), tp: 4 (over x, core).
Axes of the slice: x: 2, y: 2, z: 4, core: 2. Of those that a mesh axis runs over, the one named last changes fastest.
Arguments:
- tokens: bfloat16 [32, 4096], P(None, 'kv'), may hold values from -40 to 40, as said below
- norm_gain: float32 [4096], P('kv'), may hold values from 0.1 to 1.9
- w_query: bfloat16 [4096, 2048], P('kv', 'tp'), may hold values from -0.09375 to 0.09375
- w_key: bfloat16 [4096, 512], P('kv', 'tp'), may hold values from -0.09375 to 0.09375
- w_value: bfloat16 [4096, 512], P('kv', 'tp'), may hold values from -0.09375 to 0.09375
- forget_weight: bfloat16 [4096, 32], replicated, may hold values from -0.09375 to 0.09375
- forget_bias: float32 [32], P('tp'), may hold values from -1 to 3
- kv_cache: bfloat16 [32, 10240, 8, 128], P(None, 'kv', 'tp'), may hold values from -6 to 6
- cum_gates: float32 [32, 32, 10240], P(None, 'tp', 'kv'), may hold values from -10500 to 0, as said below
- lengths: int32 [32], replicated, may hold values from 1 to 10240, as said below
- w_out: bfloat16 [2048, 4096], P('tp', 'kv'), may hold values from -0.25 to 0.25
Outputs:
- mixed: bfloat16 [32, 4096], P(None, 'kv')
- log_weight: float32 [32, 32], P(None, 'tp')
The draws below stay inside these ranges and needn't reach their ends.
Inputs may be any that keep to these rules, and one draw needn't show every extreme that they name: Columns of tokens come in 16 groups of equal width. `cum_gates`: each row does not rise along the positions. `lengths`: some sequence has all 10240 positions cached.
All inputs are finite; a program needn't handle non-finite values.
Results may differ from the reference program's by a relative error of at most 0.0307.
Values may be sent and summed in bfloat16 or wider, within the bound.
A program may use at most 128 MiB of HBM per device.

```python
import math
import jax
import jax.numpy as jnp
from jax import lax

D = 4096
HEADS = 32
KV_HEADS = 8
HEAD = 64
BATCH = 32
CTX_DEV = 1280
LENGTH = 10240
N_KV = 8
N_TP = 4


def draw_tokens(key, part):
    first_key, second_key, third_key = jax.random.split(key, 3)
    base = jax.random.normal(first_key, (BATCH, D), jnp.float32)
    group_scale = jnp.exp(jax.random.uniform(second_key, (16,), jnp.float32, math.log(0.3), math.log(3.0)))
    columns = jnp.repeat(group_scale, D // 16)
    values = base * columns
    return jnp.clip(values, -40.0, 40.0).astype(jnp.bfloat16)


def draw_cum_gates(key, part):
    first_key, second_key, third_key = jax.random.split(key, 3)
    shift_key = jax.random.fold_in(key, 11)
    pick_key, depth_key, forced_key = jax.random.split(shift_key, 3)
    fast_share = 0.5
    is_fast = jax.random.uniform(first_key, (BATCH, HEADS), jnp.float32) < fast_share
    rate = jnp.where(is_fast, 1.0 / 30.0, 1.0 / LENGTH)
    block_factor = jnp.exp(jax.random.uniform(second_key, (BATCH, HEADS, LENGTH // CTX_DEV), jnp.float32, math.log(0.35), math.log(2.8)))
    block_factor = jnp.repeat(block_factor, CTX_DEV, axis=2)
    step_size = jax.random.uniform(third_key, (BATCH, HEADS, LENGTH), jnp.float32, 0.2, 1.8)
    log_forget = -rate[:, :, None] * block_factor * step_size
    shifted = jax.random.uniform(pick_key, (BATCH, HEADS), jnp.float32) < 0.25
    depth = jax.random.uniform(depth_key, (BATCH, HEADS), jnp.float32, 120.0, 260.0)
    forced = jax.random.randint(forced_key, (), 0, BATCH * HEADS)
    flat_index = jnp.arange(BATCH * HEADS, dtype=jnp.int32).reshape(BATCH, HEADS)
    offset = jnp.where(shifted, -depth, 0.0)
    offset = jnp.where(flat_index == forced, -jnp.maximum(depth, 200.0), offset)
    return jnp.cumsum(log_forget, axis=2) + offset[:, :, None]


def draw_lengths(key, part):
    first_key, second_key = jax.random.split(key)
    values = jax.random.randint(first_key, (BATCH,), 1, LENGTH + 1).astype(jnp.int32)
    chosen = jax.random.randint(second_key, (), 0, BATCH)
    return values.at[chosen].set(LENGTH).astype(jnp.int32)


def level_of(key, shape, cuts, low, largest):
    gain = 1.0
    for axis_at, blocks in cuts:
        draws = jax.random.uniform(jax.random.fold_in(jax.random.fold_in(key, 6), axis_at), (blocks,), jnp.float32, low / len(cuts), largest / len(cuts))
        gain = gain * jnp.repeat(jnp.exp(draws), shape[axis_at] // blocks).reshape((-1,) + (1,) * (len(shape) - 1 - axis_at))
    return gain


def noise(rng, dims, scale, most, cuts=(), kind=jnp.bfloat16):
    entries = jax.random.normal(rng, dims, jnp.float32) * scale
    if len(cuts) > 0:
        entries = level_of(rng, dims, cuts, -0.22, 0.18) * entries
    return jnp.clip(entries, min=-most, max=most).astype(kind)


def setup_inputs(seed: int = 0) -> dict:
    key_list = jax.random.split(jax.random.key(seed), 12)
    tokens = draw_tokens(jax.random.fold_in(key_list[11], 71), 0)
    norm_gain = jnp.clip(1.0 + 0.18 * jax.random.normal(key_list[1], (D,), jnp.float32), 0.1, 1.9)
    w_query = noise(key_list[2], (D, HEADS * HEAD), D ** -0.5, 0.09375, ((0, 8), (1, 4)))
    w_key = noise(key_list[3], (D, KV_HEADS * HEAD), D ** -0.5, 0.09375, ((0, 8), (1, 4)))
    w_value = noise(key_list[4], (D, KV_HEADS * HEAD), D ** -0.5, 0.09375, ((0, 8), (1, 4)))
    forget_weight = noise(key_list[5], (D, HEADS), D ** -0.5, 0.09375)
    forget_bias = jnp.clip(-1.0 + 4.0 * jax.random.uniform(key_list[6], (HEADS,), jnp.float32) ** level_of(key_list[6], (HEADS,), ((0, 4),), -0.2, 0.2), -1.0, 3.0)
    kv_cache = noise(key_list[7], (BATCH, LENGTH, KV_HEADS, 2 * HEAD), 1.0, 6.0, ((1, 8), (2, 4)))
    cum_gates = draw_cum_gates(jax.random.fold_in(key_list[11], 71), 0)
    lengths = draw_lengths(jax.random.fold_in(key_list[11], 71), 0)
    w_out = noise(key_list[10], (HEADS * HEAD, D), (HEAD * 8) ** -0.5, 0.25, ((0, 4), (1, 8)))
    return dict(tokens=tokens, norm_gain=norm_gain, w_query=w_query, w_key=w_key, w_value=w_value, forget_weight=forget_weight, forget_bias=forget_bias, kv_cache=kv_cache, cum_gates=cum_gates, lengths=lengths, w_out=w_out)


norm_eps = 1e-05
masked_floor = -1e+30

def reference(tokens, norm_gain, w_query, w_key, w_value, forget_weight, forget_bias, kv_cache, cum_gates, lengths, w_out):
    tokens_f = tokens.astype(jnp.float32)
    row_scale = lax.rsqrt(lax.optimization_barrier(jnp.mean(tokens_f * tokens_f, axis=1)) + norm_eps)[:, None]
    normalized_input = (tokens_f * norm_gain).astype(jnp.bfloat16)
    query = (row_scale * jnp.dot(normalized_input, w_query, preferred_element_type=jnp.float32)).astype(jnp.bfloat16)
    fresh_key_row = (row_scale * jnp.dot(normalized_input, w_key, preferred_element_type=jnp.float32)).astype(jnp.bfloat16)
    value_new = (row_scale * jnp.dot(normalized_input, w_value, preferred_element_type=jnp.float32)).astype(jnp.bfloat16)
    log_gate = jax.nn.log_sigmoid(row_scale * jnp.dot(normalized_input, forget_weight, preferred_element_type=jnp.float32) + forget_bias)
    group_size = HEADS // KV_HEADS
    inv_root = HEAD ** (-0.5)

    def one_row(items):
        query_row, key_row, value_row, forget_gate_row, cache_row, cum_row, length = items
        query_head_rows = query_row.astype(jnp.float32).reshape(KV_HEADS, group_size, HEAD)
        cached_keys = cache_row[:, :, :HEAD].astype(jnp.float32)
        cached_vals = cache_row[:, :, HEAD:].astype(jnp.float32)
        scores = jnp.einsum('kgd,lkd->kgl', query_head_rows, cached_keys) * inv_root
        biased = scores - cum_row.reshape(KV_HEADS, group_size, LENGTH)
        last_cum = lax.dynamic_index_in_dim(cum_row, (length - 1).astype(jnp.int32), axis=1, keepdims=False)
        cum_query = last_cum + forget_gate_row
        key_heads = key_row.astype(jnp.float32).reshape(KV_HEADS, HEAD)
        new_biased = jnp.einsum('kgd,kd->kg', query_head_rows, key_heads) * inv_root - cum_query.reshape(KV_HEADS, group_size)
        blocked = biased.reshape(KV_HEADS, group_size, N_KV, CTX_DEV)
        in_range = (jnp.arange(LENGTH, dtype=jnp.int32) < length).reshape(N_KV, CTX_DEV)
        holds_last = jnp.arange(N_KV, dtype=jnp.int32) == (length - 1) // CTX_DEV
        block_peak = lax.optimization_barrier(jnp.max(jnp.where(in_range, blocked, masked_floor), axis=-1))
        block_peak = jnp.where(holds_last, jnp.maximum(block_peak, new_biased[..., None]), block_peak)
        weights = jnp.where(in_range, jnp.exp(blocked - block_peak[..., None]), 0.0)
        new_weight = jnp.where(holds_last, jnp.exp(new_biased[..., None] - block_peak), 0.0)
        block_sum = lax.optimization_barrier(jnp.sum(weights, axis=-1)) + new_weight
        rounded = lax.optimization_barrier(weights.astype(jnp.bfloat16)).astype(jnp.float32)
        rounded_new = lax.optimization_barrier(new_weight.astype(jnp.bfloat16)).astype(jnp.float32)
        value_block_rows = jnp.einsum('kgnl,nlkd->kgnd', rounded, cached_vals.reshape(N_KV, CTX_DEV, KV_HEADS, HEAD))
        value_heads = value_row.astype(jnp.float32).reshape(KV_HEADS, 1, 1, HEAD)
        value_block_rows = value_block_rows + rounded_new[..., None] * value_heads
        peak = lax.optimization_barrier(jnp.max(block_peak, axis=-1))
        rescale_factor = jnp.exp(block_peak - peak[..., None])
        weight_sum = lax.optimization_barrier(jnp.sum(block_sum * rescale_factor, axis=-1))
        values = lax.optimization_barrier(jnp.sum(value_block_rows * rescale_factor[..., None], axis=2))
        attended = (values / weight_sum[..., None]).astype(jnp.bfloat16).reshape(HEADS * HEAD)
        log_weight = (peak + jnp.log(weight_sum)).reshape(HEADS) + cum_query
        return (attended, log_weight)
    attended, log_weight = lax.map(one_row, (query, fresh_key_row, value_new, log_gate, kv_cache, cum_gates, lengths))
    group_cols = HEADS * HEAD // N_TP
    pieces = attended.astype(jnp.float32).reshape(BATCH, N_TP, group_cols)
    out_rows = w_out.astype(jnp.float32).reshape(N_TP, group_cols, D)
    partial_out = jnp.einsum('bgc,gcd->gbd', pieces, out_rows).astype(jnp.bfloat16)
    partial_out = lax.optimization_barrier(partial_out)
    mixed = lax.optimization_barrier(jnp.sum(partial_out.astype(jnp.float32), axis=0)).astype(jnp.bfloat16)
    return (mixed, log_weight)
```

```python
import functools
import jax
import jax.numpy as jnp
from jax import lax
from jax.experimental import pallas as pl
from jax.experimental.pallas import tpu as pltpu
from jax.sharding import PartitionSpec as P

norm_eps = 1e-05
masked_floor = -1e30
LANES = 128
MESH = pl.DeviceIdType.MESH


def flip(index, step, count):
    out = index
    bit = 1
    while bit < count:
        out = out + bit * ((step // bit) % 2) * (1 - 2 * ((index // bit) % 2))
        bit *= 2
    return out


def lane_of(shape):
    return lax.broadcasted_iota(jnp.int32, shape, len(shape) - 1)


def kernel(
    n_kv,
    n_tp,
    tokens_ref,
    gain_ref,
    bias_ref,
    lengths_ref,
    w_query_hbm,
    w_key_hbm,
    w_value_hbm,
    gate_hbm,
    cache_hbm,
    cum_hbm,
    w_out_hbm,
    mixed_ref,
    log_ref,
    w_query_ref,
    w_key_ref,
    w_value_ref,
    gate_ref,
    cache_ref,
    cum_ref,
    w_out_ref,
    shift_ref,
    last_ref,
    proj_ref,
    rs1_ref,
    query_ref,
    wide_ref,
    own_query_ref,
    own_key_ref,
    own_value_ref,
    own_gate_ref,
    part_ref,
    rs2_ref,
    comb_ref,
    att_ref,
    rows_ref,
    tp_ref,
    weight_sems,
    cache_sems,
    rs1_send,
    rs1_recv,
    ag1_send,
    ag1_recv,
    rs2_send,
    rs2_recv,
    ag2_send,
    ag2_recv,
    tp_send,
    tp_recv,
):
    f32, bf16 = jnp.float32, jnp.bfloat16
    me = lax.axis_index("kv")
    my_tp = lax.axis_index("tp")
    rows, cols = tokens_ref.shape
    heads = cum_ref.shape[1]
    span = cum_ref.shape[2]
    kv_local = cache_ref.shape[1] // span
    group = heads // kv_local
    head_size = LANES // 2
    all_heads = gate_hbm.shape[0]
    mine = rows // n_kv
    q_cols = w_query_ref.shape[1]
    k_cols = w_key_ref.shape[1]
    k_pad = -(-k_cols // LANES) * LANES
    model_width = cols * n_kv
    inv_root = head_size ** (-0.5)

    gate_ref[...] = jnp.zeros_like(gate_ref)
    offset = pl.multiple_of(me * cols, cols)
    loads = [
        pltpu.make_async_copy(src, dst, weight_sems.at[i])
        for i, (src, dst) in enumerate(
            [
                (w_query_hbm, w_query_ref),
                (w_key_hbm, w_key_ref),
                (w_value_hbm, w_value_ref),
                (gate_hbm.at[:, pl.ds(offset, cols)], gate_ref.at[pl.ds(0, all_heads)]),
                (cum_hbm, cum_ref),
                (w_out_hbm, w_out_ref),
            ]
        )
    ]
    for load in loads[:5]:
        load.start()

    def cache_load(owner):
        at = pl.ds(owner * mine, mine)
        return pltpu.make_async_copy(cache_hbm.at[at], cache_ref.at[at], cache_sems.at[owner])

    for step in range(n_kv):
        cache_load(flip(me, step, n_kv)).start()
    loads[5].start()

    barrier = pltpu.get_barrier_semaphore()
    for step in range(1, n_kv):
        pl.semaphore_signal(
            barrier, inc=1, device_id={"kv": flip(me, step, n_kv)}, device_id_type=MESH
        )
    for step in range(1, n_tp):
        pl.semaphore_signal(
            barrier, inc=1, device_id={"tp": flip(my_tp, step, n_tp)}, device_id_type=MESH
        )

    tokens_f = tokens_ref[...].astype(f32)
    squares = jnp.sum(tokens_f * tokens_f, axis=1, keepdims=True)
    normed = (tokens_f * gain_ref[...]).astype(bf16)
    for load in loads[:4]:
        load.wait()
    pieces = [jnp.dot(normed, w_query_ref[...], preferred_element_type=f32)]
    for w_ref in (w_key_ref, w_value_ref):
        piece = jnp.dot(normed, w_ref[...], preferred_element_type=f32)
        if k_pad > k_cols:
            piece = jnp.concatenate([piece, jnp.zeros((rows, k_pad - k_cols), f32)], axis=1)
        pieces.append(piece)
    gates = lax.dot_general(
        normed, gate_ref[...], (((1,), (1,)), ((), ())), preferred_element_type=f32
    )
    pieces.append(jnp.where(lane_of(gates.shape) == all_heads, squares, gates))
    at = 0
    for piece in pieces:
        for owner in range(n_kv):
            proj_ref[owner, :, at : at + piece.shape[1]] = piece[
                owner * mine : (owner + 1) * mine
            ].astype(bf16)
        at += piece.shape[1]

    pl.semaphore_wait(barrier, n_kv + n_tp - 2)

    def rs1_copy(source, target):
        return pltpu.make_async_remote_copy(
            src_ref=proj_ref.at[target],
            dst_ref=rs1_ref.at[source],
            send_sem=rs1_send.at[target],
            recv_sem=rs1_recv.at[source],
            device_id={"kv": target},
            device_id_type=MESH,
        )

    for step in reversed(range(1, n_kv)):
        rs1_copy(me, flip(me, step, n_kv)).start()

    loads[4].wait()
    tile = (heads, LANES)
    lane = lane_of(tile)
    own_column = (lane % kv_local) == (lax.broadcasted_iota(jnp.int32, tile, 0) // group)

    def prepare(row, carry):
        length = lengths_ref[row] - me * span
        last = jnp.zeros(tile, f32)
        for chunk in range(span // LANES):
            cum = cum_ref[row, :, chunk * LANES : (chunk + 1) * LANES]
            place = lane + chunk * LANES
            shift = jnp.where(place < length, -cum, masked_floor)
            last = last + jnp.where(place == length - 1, cum, 0.0)
            for part in range(kv_local):
                if kv_local == 1:
                    spread = shift
                else:
                    pick = lane // kv_local + part * (LANES // kv_local)
                    spread = jnp.take_along_axis(shift, pick, axis=1)
                    spread = jnp.where(own_column, spread, masked_floor)
                at = (chunk * kv_local + part) * LANES
                shift_ref[row, :, at : at + LANES] = spread
        last_ref[row] = jnp.broadcast_to(jnp.sum(last, axis=1, keepdims=True), tile)
        return carry

    lax.fori_loop(0, rows, prepare, 0, unroll=4)

    total = proj_ref[me].astype(f32)
    for step in range(1, n_kv):
        other = flip(me, step, n_kv)
        rs1_copy(other, me).wait_recv()
        total = total + rs1_ref[other].astype(f32)
    misc = total[:, q_cols + 2 * k_pad :]
    misc_lane = lane_of(misc.shape)
    total_sq = jnp.sum(jnp.where(misc_lane == all_heads, misc, 0.0), axis=1, keepdims=True)
    row_scale = lax.rsqrt(total_sq / model_width + norm_eps)
    query_ref[me] = (row_scale * total[:, :q_cols]).astype(bf16)

    def ag1_copy(source, target):
        return pltpu.make_async_remote_copy(
            src_ref=query_ref.at[source],
            dst_ref=query_ref.at[source],
            send_sem=ag1_send.at[target],
            recv_sem=ag1_recv.at[source],
            device_id={"kv": target},
            device_id_type=MESH,
        )

    for step in reversed(range(1, n_kv)):
        ag1_copy(me, flip(me, step, n_kv)).start()

    part_lane = lane_of((mine, LANES))

    def spread_heads(ref, values, which, upper):
        for head in range(heads):
            at = which(head)
            pair = values[:, (at // 2) * LANES : (at // 2 + 1) * LANES]
            if (at % 2 == 1) != upper:
                pair = pltpu.roll(pair, head_size, 1)
            keep = (part_lane >= head_size) if upper else (part_lane < head_size)
            ref[pl.ds(head, mine, stride=heads), :] = jnp.where(keep, pair, 0.0)

    new_kv = (row_scale * total[:, q_cols : q_cols + 2 * k_pad]).astype(bf16).astype(f32)
    spread_heads(own_query_ref, query_ref[me].astype(f32), lambda head: head, False)
    spread_heads(own_key_ref, new_kv[:, :k_pad], lambda head: head // group, False)
    spread_heads(own_value_ref, new_kv[:, k_pad:], lambda head: head // group, True)
    for head in range(heads):
        own_gate_ref[pl.ds(head, mine, stride=heads), :] = row_scale * misc

    def rs2_copy(source, target):
        return pltpu.make_async_remote_copy(
            src_ref=part_ref.at[target],
            dst_ref=rs2_ref.at[source],
            send_sem=rs2_send.at[target],
            recv_sem=rs2_recv.at[source],
            device_id={"kv": target},
            device_id_type=MESH,
        )

    length_cols = cache_ref.shape[1]
    chunk_cols = 2 * LANES
    zeros = jnp.zeros((heads, LANES), f32)

    def attend(step, carry):
        owner = flip(me, step, n_kv)

        @pl.when(step > 0)
        def _():
            ag1_copy(owner, me).wait_recv()

        cache_load(owner).wait()
        spread_heads(wide_ref, query_ref[owner].astype(f32) * inv_root, lambda head: head, False)
        for pair in range(mine // 2):
            first, second = 2 * pair, 2 * pair + 1
            row_a, row_b = owner * mine + first, owner * mine + second
            left = wide_ref[first * heads : (first + 1) * heads, :]
            right = wide_ref[second * heads : (second + 1) * heads, :]
            queries = jnp.concatenate(
                [
                    jnp.concatenate([left, zeros], axis=1),
                    jnp.concatenate([zeros, right], axis=1),
                ],
                axis=0,
            ).astype(bf16)

            def entries(at):
                return jnp.concatenate(
                    [cache_ref[row_a, at : at + chunk_cols, :], cache_ref[row_b, at : at + chunk_cols, :]],
                    axis=1,
                )

            biased = []
            peak = None
            for at in range(0, length_cols, chunk_cols):
                score = lax.dot_general(
                    queries, entries(at), (((1,), (1,)), ((), ())), preferred_element_type=f32
                )
                score = score + jnp.concatenate(
                    [shift_ref[row_a, :, at : at + chunk_cols], shift_ref[row_b, :, at : at + chunk_cols]],
                    axis=0,
                )
                biased.append(score)
                peak = score if peak is None else jnp.maximum(peak, score)
            peak = jnp.max(peak, axis=1, keepdims=True)
            sums = jnp.zeros((2 * heads, chunk_cols), f32)
            values = jnp.zeros((2 * heads, chunk_cols), f32)
            for i, at in enumerate(range(0, length_cols, chunk_cols)):
                weight = jnp.exp(biased[i] - peak)
                sums = sums + weight
                values = values + jnp.dot(
                    weight.astype(bf16), entries(at), preferred_element_type=f32
                )
            total_weight = jnp.sum(sums, axis=1, keepdims=True)
            for i, (place, row) in enumerate(((first, row_a), (second, row_b))):
                inside = slice(i * heads, (i + 1) * heads)
                out = values[inside, i * LANES : (i + 1) * LANES]
                out = jnp.where(lane == 0, peak[inside], out)
                out = jnp.where(lane == 1, total_weight[inside], out)
                out = jnp.where(lane == 2, last_ref[row], out)
                part_ref[owner, place * heads : (place + 1) * heads, :] = out

        @pl.when(step > 0)
        def _():
            rs2_copy(me, owner).start()

        return carry

    lax.fori_loop(0, n_kv, attend, 0)

    tall = (mine * heads, LANES)
    tall_lane = lane_of(tall)
    head_of = lax.broadcasted_iota(jnp.int32, tall, 0) % heads
    gate = jnp.sum(
        jnp.where(tall_lane == my_tp * heads + head_of, own_gate_ref[...], 0.0),
        axis=1,
        keepdims=True,
    )
    short = (mine * heads, heads)
    gate_bias = jnp.sum(
        jnp.where(
            lane_of(short) == lax.broadcasted_iota(jnp.int32, short, 0) % heads,
            jnp.broadcast_to(bias_ref[...], short),
            0.0,
        ),
        axis=1,
        keepdims=True,
    )
    gate = gate + gate_bias
    log_gate = jnp.minimum(gate, 0.0) - jnp.log1p(jnp.exp(-jnp.abs(gate)))
    new_score = (
        jnp.sum(own_query_ref[...] * own_key_ref[...], axis=1, keepdims=True) * inv_root
    )
    blocks = [part_ref[me]]
    for step in range(1, n_kv):
        other = flip(me, step, n_kv)
        rs2_copy(other, me).wait_recv()
        blocks.append(rs2_ref[other])
    last = blocks[0]
    for block in blocks[1:]:
        last = last + block
    cum_query = last[:, 2:3] + log_gate
    new_biased = new_score - cum_query
    peak = blocks[0]
    for block in blocks[1:]:
        peak = jnp.maximum(peak, block)
    peak = jnp.maximum(peak[:, 0:1], new_biased)
    new_weight = jnp.exp(new_biased - peak)
    values = new_weight.astype(bf16).astype(f32) * own_value_ref[...]
    for block in blocks:
        values = values + jnp.exp(block[:, 0:1] - peak) * block
    weight_sum = values[:, 1:2] + new_weight
    log_weight = peak + jnp.log(weight_sum) + cum_query
    comb_ref[...] = jnp.where(tall_lane < head_size, log_weight, values / weight_sum)

    tail = jnp.zeros((mine, LANES), f32)
    even = None
    for head in range(heads):
        row = comb_ref[pl.ds(head, mine, stride=heads), :]
        tail = jnp.where((part_lane == head) | (part_lane == heads + head), row, tail)
        if head % 2 == 0:
            even = pltpu.roll(row, head_size, 1)
        else:
            at = (head // 2) * LANES
            att_ref[me, :, at : at + LANES] = jnp.where(
                part_lane < head_size, even, row
            ).astype(bf16)
    coarse = tail.astype(bf16).astype(f32)
    att_ref[me, :, q_cols:] = jnp.where(part_lane < heads, coarse, tail - coarse).astype(bf16)

    def ag2_copy(source, target):
        return pltpu.make_async_remote_copy(
            src_ref=att_ref.at[source],
            dst_ref=att_ref.at[source],
            send_sem=ag2_send.at[target],
            recv_sem=ag2_recv.at[source],
            device_id={"kv": target},
            device_id_type=MESH,
        )

    for step in reversed(range(1, n_kv)):
        ag2_copy(me, flip(me, step, n_kv)).start()
    loads[5].wait()
    for step in range(1, n_kv):
        ag2_copy(flip(me, step, n_kv), me).wait_recv()
    for owner in range(n_kv):
        rows_ref[owner * mine : (owner + 1) * mine, :] = att_ref[owner].astype(f32)
    attended = rows_ref[:, :q_cols].astype(bf16)
    tp_ref[my_tp] = jnp.dot(attended, w_out_ref[...], preferred_element_type=f32).astype(bf16)

    def tp_copy(source, target):
        return pltpu.make_async_remote_copy(
            src_ref=tp_ref.at[source],
            dst_ref=tp_ref.at[source],
            send_sem=tp_send.at[target],
            recv_sem=tp_recv.at[source],
            device_id={"tp": target},
            device_id_type=MESH,
        )

    for step in reversed(range(1, n_tp)):
        tp_copy(my_tp, flip(my_tp, step, n_tp)).start()
    tails = rows_ref[:, q_cols:]
    log_ref[...] = tails[:, :heads] + tails[:, heads : 2 * heads]

    for step in range(1, n_kv):
        other = flip(me, step, n_kv)
        rs1_copy(me, other).wait_send()
        ag1_copy(me, other).wait_send()
        rs2_copy(me, other).wait_send()
        ag2_copy(me, other).wait_send()
    for step in range(1, n_tp):
        tp_copy(flip(my_tp, step, n_tp), my_tp).wait_recv()
    mixed = tp_ref[0].astype(f32)
    for source in range(1, n_tp):
        mixed = mixed + tp_ref[source].astype(f32)
    mixed_ref[...] = mixed.astype(bf16)
    for step in range(1, n_tp):
        tp_copy(my_tp, flip(my_tp, step, n_tp)).wait_send()


def shards(
    tokens,
    norm_gain,
    w_query,
    w_key,
    w_value,
    forget_weight,
    forget_bias,
    kv_cache,
    cum_gates,
    lengths,
    w_out,
):
    n_kv, n_tp = lax.axis_size("kv"), lax.axis_size("tp")
    rows, cols = tokens.shape
    span, kv_local, entry = kv_cache.shape[1:]
    heads = cum_gates.shape[1]
    q_cols, k_cols = w_query.shape[1], w_key.shape[1]
    k_pad = -(-k_cols // LANES) * LANES
    wide = q_cols + 2 * k_pad + LANES
    mine = rows // n_kv
    out_cols = w_out.shape[1]
    f32, bf16 = jnp.float32, jnp.bfloat16
    vmem = pl.BlockSpec(memory_space=pltpu.VMEM)
    smem = pl.BlockSpec(memory_space=pltpu.SMEM)
    hbm = pl.BlockSpec(memory_space=pl.ANY)
    dma = pltpu.SemaphoreType.DMA
    tall = (mine * heads, LANES)
    return pl.pallas_call(
        functools.partial(kernel, n_kv, n_tp),
        out_shape=(
            jax.ShapeDtypeStruct((rows, out_cols), bf16),
            jax.ShapeDtypeStruct((rows, heads), f32),
        ),
        in_specs=[vmem, vmem, vmem, smem] + [hbm] * 7,
        out_specs=(vmem, vmem),
        scratch_shapes=[
            pltpu.VMEM(w_query.shape, bf16),
            pltpu.VMEM(w_key.shape, bf16),
            pltpu.VMEM(w_value.shape, bf16),
            pltpu.VMEM((LANES, cols), bf16),
            pltpu.VMEM((rows, span * kv_local, entry), bf16),
            pltpu.VMEM(cum_gates.shape, f32),
            pltpu.VMEM(w_out.shape, bf16),
            pltpu.VMEM((rows, heads, span * kv_local), f32),
            pltpu.VMEM((rows, heads, LANES), f32),
            pltpu.VMEM((n_kv, mine, wide), bf16),
            pltpu.VMEM((n_kv, mine, wide), bf16),
            pltpu.VMEM((n_kv, mine, q_cols), bf16),
            pltpu.VMEM(tall, f32),
            pltpu.VMEM(tall, f32),
            pltpu.VMEM(tall, f32),
            pltpu.VMEM(tall, f32),
            pltpu.VMEM(tall, f32),
            pltpu.VMEM((n_kv,) + tall, f32),
            pltpu.VMEM((n_kv,) + tall, f32),
            pltpu.VMEM(tall, f32),
            pltpu.VMEM((n_kv, mine, q_cols + LANES), bf16),
            pltpu.VMEM((rows, q_cols + LANES), f32),
            pltpu.VMEM((n_tp, rows, out_cols), bf16),
            dma((6,)),
            dma((n_kv,)),
        ]
        + [dma((n_kv,))] * 8
        + [dma((n_tp,))] * 2,
        compiler_params=pltpu.CompilerParams(
            collective_id=0, has_side_effects=True, vmem_limit_bytes=56 * 1024 * 1024
        ),
    )(
        tokens,
        norm_gain.reshape(1, cols),
        forget_bias.reshape(1, heads),
        lengths,
        w_query,
        w_key,
        w_value,
        forget_weight.T,
        kv_cache.reshape(rows, span * kv_local, entry),
        cum_gates,
        w_out,
    )


def solution(mesh):
    placed = (
        P(None, "kv"),
        P("kv"),
        P("kv", "tp"),
        P("kv", "tp"),
        P("kv", "tp"),
        P(),
        P("tp"),
        P(None, "kv", "tp", None),
        P(None, "tp", "kv"),
        P(),
        P("tp", "kv"),
    )
    return jax.shard_map(
        shards,
        mesh=mesh,
        in_specs=placed,
        out_specs=(P(None, "kv"), P(None, "tp")),
        check_vma=False,
    )
```

```python
import functools
import jax
import jax.numpy as jnp
from jax import lax
from jax.experimental import pallas as pl
from jax.experimental.pallas import tpu as pltpu
from jax.sharding import PartitionSpec as P

norm_eps = 1e-05
masked_floor = -1e30
LANES = 128
MESH = pl.DeviceIdType.MESH


def flip(index, step, count):
    out = index
    bit = 1
    while bit < count:
        out = out + bit * ((step // bit) % 2) * (1 - 2 * ((index // bit) % 2))
        bit *= 2
    return out


def lane_of(shape):
    return lax.broadcasted_iota(jnp.int32, shape, len(shape) - 1)


def kernel(
    n_kv,
    n_tp,
    tokens_ref,
    gain_ref,
    bias_ref,
    lengths_ref,
    w_query_hbm,
    w_key_hbm,
    w_value_hbm,
    gate_hbm,
    cache_hbm,
    cum_hbm,
    w_out_hbm,
    mixed_ref,
    log_ref,
    w_query_ref,
    w_key_ref,
    w_value_ref,
    gate_ref,
    cache_ref,
    cum_ref,
    w_out_ref,
    shift_ref,
    last_ref,
    proj_ref,
    rs1_ref,
    query_ref,
    wide_ref,
    score_ref,
    peak_ref,
    own_query_ref,
    own_key_ref,
    own_value_ref,
    own_gate_ref,
    part_ref,
    rs2_ref,
    comb_ref,
    att_ref,
    rows_ref,
    tp_ref,
    weight_sems,
    cache_sems,
    rs1_send,
    rs1_recv,
    ag1_send,
    ag1_recv,
    rs2_send,
    rs2_recv,
    ag2_send,
    ag2_recv,
    tp_send,
    tp_recv,
):
    f32, bf16 = jnp.float32, jnp.bfloat16
    me = lax.axis_index("kv")
    my_tp = lax.axis_index("tp")
    rows, cols = tokens_ref.shape
    heads = cum_ref.shape[1]
    span = cum_ref.shape[2]
    kv_local = cache_ref.shape[1] // span
    group = heads // kv_local
    head_size = LANES // 2
    all_heads = gate_hbm.shape[0]
    mine = rows // n_kv
    q_cols = w_query_ref.shape[1]
    k_cols = w_key_ref.shape[1]
    k_pad = -(-k_cols // LANES) * LANES
    model_width = cols * n_kv
    inv_root = head_size ** (-0.5)

    gate_ref[...] = jnp.zeros_like(gate_ref)
    offset = pl.multiple_of(me * cols, cols)
    loads = [
        pltpu.make_async_copy(src, dst, weight_sems.at[i])
        for i, (src, dst) in enumerate(
            [
                (w_query_hbm, w_query_ref),
                (w_key_hbm, w_key_ref),
                (w_value_hbm, w_value_ref),
                (gate_hbm.at[:, pl.ds(offset, cols)], gate_ref.at[pl.ds(0, all_heads)]),
                (cum_hbm, cum_ref),
                (w_out_hbm, w_out_ref),
            ]
        )
    ]
    for load in loads[:5]:
        load.start()

    def cache_load(owner):
        at = pl.ds(owner * mine, mine)
        return pltpu.make_async_copy(cache_hbm.at[at], cache_ref.at[at], cache_sems.at[owner])

    barrier = pltpu.get_barrier_semaphore()
    for step in range(1, n_kv):
        pl.semaphore_signal(
            barrier, inc=1, device_id={"kv": flip(me, step, n_kv)}, device_id_type=MESH
        )
    for step in range(1, n_tp):
        pl.semaphore_signal(
            barrier, inc=1, device_id={"tp": flip(my_tp, step, n_tp)}, device_id_type=MESH
        )

    tokens_f = tokens_ref[...].astype(f32)
    squares = jnp.sum(tokens_f * tokens_f, axis=1, keepdims=True)
    normed = (tokens_f * gain_ref[...]).astype(bf16)
    for load in loads[:4]:
        load.wait()
    for step in range(n_kv):
        cache_load(flip(me, step, n_kv)).start()
    loads[5].start()
    pieces = [jnp.dot(normed, w_query_ref[...], preferred_element_type=f32)]
    for w_ref in (w_key_ref, w_value_ref):
        piece = jnp.dot(normed, w_ref[...], preferred_element_type=f32)
        if k_pad > k_cols:
            piece = jnp.concatenate([piece, jnp.zeros((rows, k_pad - k_cols), f32)], axis=1)
        pieces.append(piece)
    gates = lax.dot_general(
        normed, gate_ref[...], (((1,), (1,)), ((), ())), preferred_element_type=f32
    )
    pieces.append(jnp.where(lane_of(gates.shape) == all_heads, squares, gates))
    at = 0
    for piece in pieces:
        for owner in range(n_kv):
            proj_ref[owner, :, at : at + piece.shape[1]] = piece[
                owner * mine : (owner + 1) * mine
            ].astype(bf16)
        at += piece.shape[1]

    pl.semaphore_wait(barrier, n_kv + n_tp - 2)

    def rs1_copy(source, target):
        return pltpu.make_async_remote_copy(
            src_ref=proj_ref.at[target],
            dst_ref=rs1_ref.at[source],
            send_sem=rs1_send.at[target],
            recv_sem=rs1_recv.at[source],
            device_id={"kv": target},
            device_id_type=MESH,
        )

    for step in reversed(range(1, n_kv)):
        rs1_copy(me, flip(me, step, n_kv)).start()

    loads[4].wait()
    tile = (heads, LANES)
    lane = lane_of(tile)
    own_column = (lane % kv_local) == (lax.broadcasted_iota(jnp.int32, tile, 0) // group)

    def prepare(row, carry):
        length = lengths_ref[row] - me * span
        last = jnp.zeros(tile, f32)
        for chunk in range(span // LANES):
            cum = cum_ref[row, :, chunk * LANES : (chunk + 1) * LANES]
            place = lane + chunk * LANES
            shift = jnp.where(place < length, -cum, masked_floor)
            last = last + jnp.where(place == length - 1, cum, 0.0)
            for part in range(kv_local):
                if kv_local == 1:
                    spread = shift
                else:
                    pick = lane // kv_local + part * (LANES // kv_local)
                    spread = jnp.take_along_axis(shift, pick, axis=1)
                    spread = jnp.where(own_column, spread, masked_floor)
                at = (chunk * kv_local + part) * LANES
                shift_ref[row, :, at : at + LANES] = spread
        last_ref[row] = jnp.broadcast_to(jnp.sum(last, axis=1, keepdims=True), tile)
        return carry

    lax.fori_loop(0, rows, prepare, 0, unroll=4)

    total = proj_ref[me].astype(f32)
    for step in range(1, n_kv):
        other = flip(me, step, n_kv)
        rs1_copy(other, me).wait_recv()
        total = total + rs1_ref[other].astype(f32)
    misc = total[:, q_cols + 2 * k_pad :]
    misc_lane = lane_of(misc.shape)
    total_sq = jnp.sum(jnp.where(misc_lane == all_heads, misc, 0.0), axis=1, keepdims=True)
    row_scale = lax.rsqrt(total_sq / model_width + norm_eps)
    query_ref[me] = (row_scale * total[:, :q_cols]).astype(bf16)

    def ag1_copy(source, target):
        return pltpu.make_async_remote_copy(
            src_ref=query_ref.at[source],
            dst_ref=query_ref.at[source],
            send_sem=ag1_send.at[target],
            recv_sem=ag1_recv.at[source],
            device_id={"kv": target},
            device_id_type=MESH,
        )

    for step in reversed(range(1, n_kv)):
        ag1_copy(me, flip(me, step, n_kv)).start()

    part_lane = lane_of((mine, LANES))

    def spread_heads(ref, values, which, upper):
        for head in range(heads):
            at = which(head)
            pair = values[:, (at // 2) * LANES : (at // 2 + 1) * LANES]
            if (at % 2 == 1) != upper:
                pair = pltpu.roll(pair, head_size, 1)
            keep = (part_lane >= head_size) if upper else (part_lane < head_size)
            ref[pl.ds(head, mine, stride=heads), :] = jnp.where(keep, pair, 0.0)

    new_kv = (row_scale * total[:, q_cols : q_cols + 2 * k_pad]).astype(bf16).astype(f32)
    spread_heads(own_query_ref, query_ref[me].astype(f32), lambda head: head, False)
    spread_heads(own_key_ref, new_kv[:, :k_pad], lambda head: head // group, False)
    spread_heads(own_value_ref, new_kv[:, k_pad:], lambda head: head // group, True)
    for head in range(heads):
        own_gate_ref[pl.ds(head, mine, stride=heads), :] = row_scale * misc

    def rs2_copy(source, target):
        return pltpu.make_async_remote_copy(
            src_ref=part_ref.at[target],
            dst_ref=rs2_ref.at[source],
            send_sem=rs2_send.at[target],
            recv_sem=rs2_recv.at[source],
            device_id={"kv": target},
            device_id_type=MESH,
        )

    length_cols = cache_ref.shape[1]
    chunk_cols = 2 * LANES
    chunks = range(0, length_cols, chunk_cols)
    zeros = jnp.zeros((heads, LANES), f32)
    pairs = range(mine // 2)

    def entries(row_a, row_b, at):
        inside = slice(at, at + chunk_cols)
        return jnp.concatenate([cache_ref[row_a, inside, :], cache_ref[row_b, inside, :]], axis=1)

    def weigh(pair):
        peak = peak_ref[pair, :, :1]
        sums = jnp.zeros((2 * heads, chunk_cols), f32)
        weights = []
        for at in chunks:
            weight = jnp.exp(score_ref[pair, :, at : at + chunk_cols] - peak)
            sums = sums + weight
            weights.append(weight.astype(bf16))
        return weights, jnp.sum(sums, axis=1, keepdims=True), peak

    def score(owner, pair):
        first, second = 2 * pair, 2 * pair + 1
        row_a, row_b = owner * mine + first, owner * mine + second
        left = wide_ref[first * heads : (first + 1) * heads, :]
        right = wide_ref[second * heads : (second + 1) * heads, :]
        queries = jnp.concatenate(
            [
                jnp.concatenate([left, zeros], axis=1),
                jnp.concatenate([zeros, right], axis=1),
            ],
            axis=0,
        ).astype(bf16)
        peak = None
        for at in chunks:
            part = lax.dot_general(
                queries,
                entries(row_a, row_b, at),
                (((1,), (1,)), ((), ())),
                preferred_element_type=f32,
            )
            part = part + jnp.concatenate(
                [shift_ref[row_a, :, at : at + chunk_cols], shift_ref[row_b, :, at : at + chunk_cols]],
                axis=0,
            )
            score_ref[pair, :, at : at + chunk_cols] = part
            peak = part if peak is None else jnp.maximum(peak, part)
        peak_ref[pair] = jnp.broadcast_to(
            jnp.max(peak, axis=1, keepdims=True), (2 * heads, LANES)
        )

    def gather(owner, pair, weights, total_weight, peak):
        first, second = 2 * pair, 2 * pair + 1
        row_a, row_b = owner * mine + first, owner * mine + second
        values = jnp.zeros((2 * heads, chunk_cols), f32)
        for weight, at in zip(weights, chunks):
            values = values + jnp.dot(
                weight, entries(row_a, row_b, at), preferred_element_type=f32
            )
        for i, (place, row) in enumerate(((first, row_a), (second, row_b))):
            inside = slice(i * heads, (i + 1) * heads)
            out = values[inside, i * LANES : (i + 1) * LANES]
            out = jnp.where(lane == 0, peak[inside], out)
            out = jnp.where(lane == 1, total_weight[inside], out)
            out = jnp.where(lane == 2, last_ref[row], out)
            part_ref[owner, place * heads : (place + 1) * heads, :] = out

    def ready(owner):
        cache_load(owner).wait()
        spread_heads(wide_ref, query_ref[owner].astype(f32) * inv_root, lambda head: head, False)

    ready(me)
    for pair in pairs:
        score(me, pair)

    def attend(step, carry):
        owner, after = flip(me, step, n_kv), flip(me, step + 1, n_kv)
        ag1_copy(after, me).wait_recv()
        ready(after)
        for pair in pairs:
            weights = weigh(pair)
            score(after, pair)
            gather(owner, pair, *weights)

        @pl.when(step > 0)
        def _():
            rs2_copy(me, owner).start()

        return carry

    lax.fori_loop(0, n_kv - 1, attend, 0)
    final = flip(me, n_kv - 1, n_kv)
    for pair in pairs:
        gather(final, pair, *weigh(pair))
    rs2_copy(me, final).start()

    tall = (mine * heads, LANES)
    tall_lane = lane_of(tall)
    head_of = lax.broadcasted_iota(jnp.int32, tall, 0) % heads
    gate = jnp.sum(
        jnp.where(tall_lane == my_tp * heads + head_of, own_gate_ref[...], 0.0),
        axis=1,
        keepdims=True,
    )
    short = (mine * heads, heads)
    gate_bias = jnp.sum(
        jnp.where(
            lane_of(short) == lax.broadcasted_iota(jnp.int32, short, 0) % heads,
            jnp.broadcast_to(bias_ref[...], short),
            0.0,
        ),
        axis=1,
        keepdims=True,
    )
    gate = gate + gate_bias
    log_gate = jnp.minimum(gate, 0.0) - jnp.log1p(jnp.exp(-jnp.abs(gate)))
    new_score = (
        jnp.sum(own_query_ref[...] * own_key_ref[...], axis=1, keepdims=True) * inv_root
    )
    blocks = [part_ref[me]]
    for step in range(1, n_kv):
        other = flip(me, step, n_kv)
        rs2_copy(other, me).wait_recv()
        blocks.append(rs2_ref[other])
    last = blocks[0]
    for block in blocks[1:]:
        last = last + block
    cum_query = last[:, 2:3] + log_gate
    new_biased = new_score - cum_query
    peak = blocks[0]
    for block in blocks[1:]:
        peak = jnp.maximum(peak, block)
    peak = jnp.maximum(peak[:, 0:1], new_biased)
    new_weight = jnp.exp(new_biased - peak)
    values = new_weight.astype(bf16).astype(f32) * own_value_ref[...]
    for block in blocks:
        values = values + jnp.exp(block[:, 0:1] - peak) * block
    weight_sum = values[:, 1:2] + new_weight
    log_weight = peak + jnp.log(weight_sum) + cum_query
    comb_ref[...] = jnp.where(tall_lane < head_size, log_weight, values / weight_sum)

    tail = jnp.zeros((mine, LANES), f32)
    even = None
    for head in range(heads):
        row = comb_ref[pl.ds(head, mine, stride=heads), :]
        tail = jnp.where((part_lane == head) | (part_lane == heads + head), row, tail)
        if head % 2 == 0:
            even = pltpu.roll(row, head_size, 1)
        else:
            at = (head // 2) * LANES
            att_ref[me, :, at : at + LANES] = jnp.where(
                part_lane < head_size, even, row
            ).astype(bf16)
    coarse = tail.astype(bf16).astype(f32)
    att_ref[me, :, q_cols:] = jnp.where(part_lane < heads, coarse, tail - coarse).astype(bf16)

    def ag2_copy(source, target):
        return pltpu.make_async_remote_copy(
            src_ref=att_ref.at[source],
            dst_ref=att_ref.at[source],
            send_sem=ag2_send.at[target],
            recv_sem=ag2_recv.at[source],
            device_id={"kv": target},
            device_id_type=MESH,
        )

    for step in reversed(range(1, n_kv)):
        ag2_copy(me, flip(me, step, n_kv)).start()
    loads[5].wait()
    for step in range(1, n_kv):
        ag2_copy(flip(me, step, n_kv), me).wait_recv()
    for owner in range(n_kv):
        rows_ref[owner * mine : (owner + 1) * mine, :] = att_ref[owner].astype(f32)
    attended = rows_ref[:, :q_cols].astype(bf16)
    tp_ref[my_tp] = jnp.dot(attended, w_out_ref[...], preferred_element_type=f32).astype(bf16)

    def tp_copy(source, target):
        return pltpu.make_async_remote_copy(
            src_ref=tp_ref.at[source],
            dst_ref=tp_ref.at[source],
            send_sem=tp_send.at[target],
            recv_sem=tp_recv.at[source],
            device_id={"tp": target},
            device_id_type=MESH,
        )

    for step in reversed(range(1, n_tp)):
        tp_copy(my_tp, flip(my_tp, step, n_tp)).start()
    tails = rows_ref[:, q_cols:]
    log_ref[...] = tails[:, :heads] + tails[:, heads : 2 * heads]

    for step in range(1, n_kv):
        other = flip(me, step, n_kv)
        rs1_copy(me, other).wait_send()
        ag1_copy(me, other).wait_send()
        rs2_copy(me, other).wait_send()
        ag2_copy(me, other).wait_send()
    for step in range(1, n_tp):
        tp_copy(flip(my_tp, step, n_tp), my_tp).wait_recv()
    mixed = tp_ref[0].astype(f32)
    for source in range(1, n_tp):
        mixed = mixed + tp_ref[source].astype(f32)
    mixed_ref[...] = mixed.astype(bf16)
    for step in range(1, n_tp):
        tp_copy(my_tp, flip(my_tp, step, n_tp)).wait_send()


def shards(
    tokens,
    norm_gain,
    w_query,
    w_key,
    w_value,
    forget_weight,
    forget_bias,
    kv_cache,
    cum_gates,
    lengths,
    w_out,
):
    n_kv, n_tp = lax.axis_size("kv"), lax.axis_size("tp")
    rows, cols = tokens.shape
    span, kv_local, entry = kv_cache.shape[1:]
    heads = cum_gates.shape[1]
    q_cols, k_cols = w_query.shape[1], w_key.shape[1]
    k_pad = -(-k_cols // LANES) * LANES
    wide = q_cols + 2 * k_pad + LANES
    mine = rows // n_kv
    out_cols = w_out.shape[1]
    f32, bf16 = jnp.float32, jnp.bfloat16
    vmem = pl.BlockSpec(memory_space=pltpu.VMEM)
    smem = pl.BlockSpec(memory_space=pltpu.SMEM)
    hbm = pl.BlockSpec(memory_space=pl.ANY)
    dma = pltpu.SemaphoreType.DMA
    tall = (mine * heads, LANES)
    return pl.pallas_call(
        functools.partial(kernel, n_kv, n_tp),
        out_shape=(
            jax.ShapeDtypeStruct((rows, out_cols), bf16),
            jax.ShapeDtypeStruct((rows, heads), f32),
        ),
        in_specs=[vmem, vmem, vmem, smem] + [hbm] * 7,
        out_specs=(vmem, vmem),
        scratch_shapes=[
            pltpu.VMEM(w_query.shape, bf16),
            pltpu.VMEM(w_key.shape, bf16),
            pltpu.VMEM(w_value.shape, bf16),
            pltpu.VMEM((LANES, cols), bf16),
            pltpu.VMEM((rows, span * kv_local, entry), bf16),
            pltpu.VMEM(cum_gates.shape, f32),
            pltpu.VMEM(w_out.shape, bf16),
            pltpu.VMEM((rows, heads, span * kv_local), f32),
            pltpu.VMEM((rows, heads, LANES), f32),
            pltpu.VMEM((n_kv, mine, wide), bf16),
            pltpu.VMEM((n_kv, mine, wide), bf16),
            pltpu.VMEM((n_kv, mine, q_cols), bf16),
            pltpu.VMEM(tall, f32),
            pltpu.VMEM((mine // 2, 2 * heads, span * kv_local), f32),
            pltpu.VMEM((mine // 2, 2 * heads, LANES), f32),
            pltpu.VMEM(tall, f32),
            pltpu.VMEM(tall, f32),
            pltpu.VMEM(tall, f32),
            pltpu.VMEM(tall, f32),
            pltpu.VMEM((n_kv,) + tall, f32),
            pltpu.VMEM((n_kv,) + tall, f32),
            pltpu.VMEM(tall, f32),
            pltpu.VMEM((n_kv, mine, q_cols + LANES), bf16),
            pltpu.VMEM((rows, q_cols + LANES), f32),
            pltpu.VMEM((n_tp, rows, out_cols), bf16),
            dma((6,)),
            dma((n_kv,)),
        ]
        + [dma((n_kv,))] * 8
        + [dma((n_tp,))] * 2,
        compiler_params=pltpu.CompilerParams(
            collective_id=0, has_side_effects=True, vmem_limit_bytes=56 * 1024 * 1024
        ),
    )(
        tokens,
        norm_gain.reshape(1, cols),
        forget_bias.reshape(1, heads),
        lengths,
        w_query,
        w_key,
        w_value,
        forget_weight.T,
        kv_cache.reshape(rows, span * kv_local, entry),
        cum_gates,
        w_out,
    )


def solution(mesh):
    placed = (
        P(None, "kv"),
        P("kv"),
        P("kv", "tp"),
        P("kv", "tp"),
        P("kv", "tp"),
        P(),
        P("tp"),
        P(None, "kv", "tp", None),
        P(None, "tp", "kv"),
        P(),
        P("tp", "kv"),
    )
    return jax.shard_map(
        shards,
        mesh=mesh,
        in_specs=placed,
        out_specs=(P(None, "kv"), P(None, "tp")),
        check_vma=False,
    )
```
